256 devices in a mesh: fs: 32 (over z, x), tp: 8 (over y, core).
Axes of the slice: x: 4, y: 4, z: 8, core: 2. Of those that a mesh axis runs over, the one named last changes fastest.
Arguments:
- saved_input: bfloat16 [393216, 2048], P(('fs', 'tp')), may hold values from -6 to 6
- value_cotangent: bfloat16 [393216, 1024], P(('fs', 'tp')), may hold values from -0.0390625 to 0.0390625
- decay_cotangent: bfloat16 [393216, 16], P(('fs', 'tp')), may hold values from -0.009765625 to 0.009765625
- value_master: float32 [2048, 1024], P('fs', 'tp'), may hold values from -6 to 6
- value_factor: bfloat16 [2048, 256], P('fs'), may hold values from -0.22097087 to 0.22097087
- value_mean: float32 [256, 1024], P('fs', 'tp'), may hold values from -0.625 to 0.625
- value_second: float32 [256, 1024], P('fs', 'tp'), may hold values from 0.0001 to 0.1
- decay_master: float32 [2048, 16], replicated, may hold values from -6 to 6
- decay_mean: float32 [2048, 16], replicated, may hold values from -0.625 to 0.625
- decay_second: float32 [2048, 16], replicated, may hold values from 0.001 to 0.01
Outputs:
- value_step: float32 [2048, 1024], P('fs', 'tp')
- value_new: float32 [2048, 1024], P('fs', 'tp')
- value_copy: bfloat16 [2048, 1024], P(None, 'tp')
- mean_new: float32 [256, 1024], P('fs', 'tp')
- second_new: float32 [256, 1024], P('fs', 'tp')
- decay_step: float32 [2048, 16], replicated
- decay_copy: bfloat16 [2048, 16], replicated
The draws below stay inside these ranges and needn't reach their ends.
All inputs are finite; a program needn't handle non-finite values.
Results may differ from the reference program's by a relative error of at most 0.0004.
Values may be sent and summed in bfloat16 or wider, within the bound.
A program may use at most 64 MiB of HBM per device.

```python
import math
import jax
import jax.numpy as jnp
from jax import lax

D = 2048
HG = 16
GW = 1024
RANK = 256
TOKENS = 393216


def draw_value_factor(key, part):
    base_key, tilt_key = jax.random.split(jax.random.fold_in(key, 17))
    base = jnp.clip(jax.random.normal(base_key, (D, RANK), jnp.float32), -4.0, 4.0)
    place = jnp.arange(D, dtype=jnp.float32)[:, None] / D
    jitter = jax.random.uniform(tilt_key, (D, 1), jnp.float32)
    scale = 10.0 ** (0.5 * place + 0.5 * jitter) * 0.25 * D ** (-0.5)
    return (base * scale).astype(jnp.bfloat16)


def draw_value_second(key, part):
    entry_key, tilt_key = jax.random.split(jax.random.fold_in(key, 29))
    place = jnp.arange(GW, dtype=jnp.float32)[None, :] / GW
    jitter = jax.random.uniform(tilt_key, (1, GW), jnp.float32)
    column = 100.0 ** (0.5 * place + 0.5 * jitter)
    entry = 10.0 ** jax.random.uniform(entry_key, (RANK, GW), jnp.float32)
    return (0.0001 * entry * column).astype(jnp.float32)


def strengthened(result, own_key, source, target, parts, factor):
    owner, partner = [(jnp.arange(result.shape[axis_at]) // (result.shape[axis_at] // parts)).reshape([-1 if axis == axis_at else 1 for axis in range(result.ndim)]) for axis_at in (source, target)]
    chosen = jax.random.permutation(own_key, parts)[partner]
    strong = (owner == chosen) | (owner == (partner + parts // 2) % parts)
    return jnp.where(strong, factor * result, result)


def shard_levels(stream_key, extent, cuts, smallest, largest):
    def one(position, blocks):
        steps = jax.random.uniform(jax.random.fold_in(jax.random.fold_in(stream_key, 6), position), (blocks,), jnp.float32, smallest / len(cuts), largest / len(cuts))
        return jnp.repeat(jnp.exp(steps), extent[position] // blocks).reshape((-1,) + (1,) * (len(extent) - position - 1))

    level = one(*cuts[0])
    for cut in cuts[1:]:
        level = level * one(*cut)
    return level


def centred(stream_key, dims, spread, reach, pieces=(), kind=jnp.bfloat16):
    drawn = spread * jax.random.normal(stream_key, dims, jnp.float32)
    if pieces:
        drawn = drawn * shard_levels(stream_key, dims, pieces, -0.22, 0.18)
    return jnp.clip(drawn, -reach, reach).astype(kind)


def bell_draw_with(own_key, extent, deviation, bound, shards, heavy, kind=jnp.bfloat16):
    drawn = deviation * jax.random.normal(own_key, extent, jnp.float32)
    if shards:
        drawn = drawn * shard_levels(own_key, extent, shards, -0.22, 0.18)
    return jnp.clip(strengthened(drawn, jax.random.fold_in(own_key, 3), *heavy), -bound, bound).astype(kind)


def setup_inputs(seed: int = 0) -> dict:
    key_list = jax.random.split(jax.random.key(seed), 11)
    return {
        "saved_input": centred(key_list[0], (TOKENS, D), 1.0, 6.0, ((0, 256),)),
        "value_cotangent": bell_draw_with(key_list[1], (TOKENS, GW), (TOKENS ** -0.5), 0.0390625, ((0, 256),), (0, 1, 256, 6.0)),
        "decay_cotangent": centred(key_list[2], (TOKENS, HG), (TOKENS ** -0.5), 0.009765625, ((0, 256),)),
        "value_master": centred(key_list[3], (D, GW), 1.0, 6.0, ((0, 32), (1, 8)), jnp.float32),
        "value_factor": draw_value_factor(jax.random.fold_in(key_list[10], 71), 0),
        "value_mean": centred(key_list[5], (RANK, GW), 0.1, 0.625, ((0, 32), (1, 8)), jnp.float32),
        "value_second": draw_value_second(jax.random.fold_in(key_list[10], 71), 0),
        "decay_master": centred(key_list[7], (D, HG), 1.0, 6.0, (), jnp.float32),
        "decay_mean": centred(key_list[8], (D, HG), 0.1, 0.625, (), jnp.float32),
        "decay_second": jnp.clip(jnp.exp(jax.random.uniform(key_list[9], (D, HG), jnp.float32, math.log(0.001), math.log(0.01))), 0.001, 0.01),
    }


BETA_ONE = 0.9
BETA_TWO = 0.99
ADAM_EPS = 1e-08
RMS_EPS = 1e-06
LEARN_RATE = 0.05
TOKEN_DIMS = (((0,), (0,)), ((), ()))

def adam_direction(moment_one, moment_two, gradient):
    mean_new = BETA_ONE * moment_one + (1.0 - BETA_ONE) * gradient
    second_new = BETA_TWO * moment_two + (1.0 - BETA_TWO) * gradient * gradient
    return (mean_new, second_new, mean_new / (jnp.sqrt(second_new) + ADAM_EPS))

def reference(saved_input, value_cotangent, decay_cotangent, value_master, value_factor, value_mean, value_second, decay_master, decay_mean, decay_second):
    value_grad = lax.dot_general(saved_input, value_cotangent, TOKEN_DIMS, preferred_element_type=jnp.float32)
    factor_wide = value_factor.astype(jnp.float32)
    projected = lax.dot_general(factor_wide, value_grad, TOKEN_DIMS, precision=lax.Precision.HIGHEST, preferred_element_type=jnp.float32)
    mean_new, second_new, direction = adam_direction(value_mean, value_second, projected)
    raw_update = jnp.dot(factor_wide, direction, precision=lax.Precision.HIGHEST, preferred_element_type=jnp.float32)
    value_step = raw_update * lax.rsqrt(jnp.mean(raw_update * raw_update) + RMS_EPS)
    value_new = value_master - LEARN_RATE * value_step
    value_copy = value_new.astype(jnp.bfloat16)
    decay_grad = lax.dot_general(saved_input, decay_cotangent, TOKEN_DIMS, preferred_element_type=jnp.float32)
    unused_mean, unused_second, decay_step = adam_direction(decay_mean, decay_second, decay_grad)
    decay_copy = (decay_master - LEARN_RATE * decay_step).astype(jnp.bfloat16)
    return (value_step, value_new, value_copy, mean_new, second_new, decay_step, decay_copy)
```

```python
import functools

import jax
import jax.numpy as jnp
from jax import lax
from jax.experimental import pallas as pl
from jax.experimental.pallas import tpu as pltpu
from jax.sharding import Mesh
from jax.sharding import PartitionSpec as P

MESH = pl.DeviceIdType.MESH
FS = ("fs_0", "fs_1")
TP = ("tp_0", "tp_1")
FS_TP = FS + TP
NZ, NX, NY, NC = 8, 4, 4, 2
D = 2048
GW = 1024
RANK = 256
HG = 16
TOK = 1536

BETA_ONE = 0.9
BETA_TWO = 0.99
ADAM_EPS = 1e-08
RMS_EPS = 1e-06
LEARN_RATE = 0.05

N_REMOTE = 7 + 6 + 8 + 7 + 3 + 24 + 4 + 3 + 3 + 7 + 7 + 3 + 7
F32 = jnp.float32
BF16 = jnp.bfloat16


def moments(mean, second, grad):
    mean_new = BETA_ONE * mean + (1.0 - BETA_ONE) * grad
    second_new = BETA_TWO * second + (1.0 - BETA_TWO) * grad * grad
    return mean_new, second_new, mean_new / (jnp.sqrt(second_new) + ADAM_EPS)


def split_two(value):
    high = value.astype(BF16)
    return high, (value - high.astype(F32)).astype(BF16)


def kernel(
    x_in, g_in, dct_in, master_in, f_in, mean_in, second_in, dmaster_in, dmean_in, dsecond_in,
    step_out, new_out, copy_out, mean_out, second_out, dstep_out, dcopy_out,
    xv, gv, dctv, fv, mv, meanv, secondv, dmasterv, dmeanv, dsecondv,
    mapped, split_t, pbuf, crecv, yrecv, sbuf, xrecv, tbuf, zrecv, dirb, ubuf, sqb,
    dacc, dbuf, dcrecv, dyrecv, dsend, dxrecv, dzall, dgrad,
    stepv, newv, copyv, dstepv, dcopyv,
    local_sem, send_sem, recv_sem,
):
    z = lax.axis_index("fs_0")
    x = lax.axis_index("fs_1")
    y = lax.axis_index("tp_0")
    c = lax.axis_index("tp_1")
    tp = y * NC + c
    mate = 1 - c
    half = pl.ds(pl.multiple_of(c * 32, 32), 32)

    def z_at(k):
        return {"fs_0": lax.rem(z + k, NZ)}

    def x_at(k):
        return {"fs_1": lax.rem(x + k, NX)}

    def y_at(k):
        return {"tp_0": lax.rem(y + k, NY)}

    def tp_at(k):
        other = lax.rem(tp + k, NY * NC)
        return {"tp_0": other // NC, "tp_1": lax.rem(other, NC)}

    core = {"tp_1": mate}
    z_far = (4, 3, 5, 2, 6, 1, 7)
    x_far = (2, 1, 3)

    locals_started = []
    sends = []

    def fetch(src, dst):
        copy = pltpu.make_async_copy(src, dst, local_sem.at[len(locals_started)])
        copy.start()
        locals_started.append(copy)
        return copy

    def send(src, dst, where):
        n = len(sends)
        copy = pltpu.make_async_remote_copy(
            src_ref=src, dst_ref=dst, send_sem=send_sem.at[n], recv_sem=recv_sem.at[n],
            device_id=where, device_id_type=MESH,
        )
        copy.start()
        sends.append(copy)
        return copy

    own_f = fetch(f_in.at[half], fv.at[z, x, half])
    dct_load = fetch(dct_in, dctv)
    x_loads = [
        fetch(x_in.at[pl.ds(512 * i, 512)], xv.at[pl.ds(512 * i, 512)]) for i in range(3)
    ]
    own_m = fetch(master_in, mv.at[z, x])
    g_load = fetch(g_in, gv)
    small_loads = [
        fetch(mean_in, meanv), fetch(second_in, secondv), fetch(dmaster_in, dmasterv),
        fetch(dmean_in, dmeanv), fetch(dsecond_in, dsecondv),
    ]

    barrier = pltpu.get_barrier_semaphore()
    peers = [z_at(k) for k in z_far] + [x_at(k) for k in x_far]
    peers += [tp_at(k) for k in range(1, 8)]
    for peer in peers:
        pl.semaphore_signal(barrier, inc=1, device_id=peer, device_id_type=MESH)
    pl.semaphore_wait(barrier, len(peers))

    own_f.wait()
    f_z = [send(fv.at[z, x, half], fv.at[z, x, half], z_at(k)) for k in z_far]

    dct_load.wait()
    for i in range(3):
        x_loads[i].wait()
        part = jnp.dot(
            dctv[:, 512 * i : 512 * (i + 1)], xv[512 * i : 512 * (i + 1), :],
            preferred_element_type=F32,
        )
        if i < 2:
            dacc[...] = part if i == 0 else dacc[...] + part
        else:
            part = dacc[...] + part
            for t in range(NY * NC):
                for q in range(NX):
                    row, col = 8 * (q // 2), 256 * t + 128 * (q % 2)
                    dbuf[t // NC, t % NC, q] = part[row : row + 8, col : col + 128]
    d_core = send(dbuf.at[:, mate], dcrecv, core)

    for copy in f_z:
        copy.wait_recv()
    zs = [pl.ds(4 * h, 4) for h in range(2)]
    f_x = [
        [send(fv.at[zs[h], x, half], fv.at[zs[h], x, half], x_at(k)) for k in x_far]
        for h in range(2)
    ]
    f_c = [[send(fv.at[zs[h], x, half], fv.at[zs[h], x, half], core)] for h in range(2)]

    d_core.wait_recv()
    for t in range(NY):
        dbuf[t, c] = dbuf[t, c] + dcrecv[t]
    d_y = [
        send(dbuf.at[lax.rem(y + k, NY), c], dyrecv.at[k - 1], y_at(k)) for k in (2, 1, 3)
    ]
    own_m.wait()
    m_z = [send(mv.at[z, x], mv.at[z, x], z_at(k)) for k in z_far]

    for copy in d_y:
        copy.wait_recv()
    dsend[...] = dbuf[y, c] + dyrecv[0] + dyrecv[1] + dyrecv[2]
    d_x = [send(dsend.at[lax.rem(x + k, NX)], dxrecv.at[k - 1], x_at(k)) for k in x_far]

    for h in range(2):
        for k in range(3):
            f_x[h][k].wait_recv()
            source = lax.rem(x + NX - x_far[k], NX)
            piece = fv.at[zs[h], source, half]
            f_c[h].append(send(piece, piece, core))
        if h == 0:
            for copy in d_x:
                copy.wait_recv()
            dzall[z] = dsend[x] + dxrecv[0] + dxrecv[1] + dxrecv[2]
            d_z = [send(dzall.at[z], dzall.at[z], z_at(k)) for k in z_far]
        for copy in f_c[h]:
            copy.wait_recv()

        def tile(i, carry):
            rows = pl.ds(pl.multiple_of(i * 256, 256), 256)
            factor = fv[4 * h : 4 * h + 4].reshape(1024, RANK)
            part = jnp.dot(
                xv[rows, 1024 * h : 1024 * (h + 1)], factor, preferred_element_type=F32
            )
            if h == 0:
                mapped[rows, :] = part
            else:
                high, low = split_two((mapped[rows, :] + part).T)
                split_t[0:256, rows] = high
                split_t[256:512, rows] = low
            return carry

        lax.fori_loop(0, TOK // 256, tile, 0)

    for copy in m_z:
        copy.wait_recv()
    m_x = [send(mv.at[:, x], mv.at[:, x], x_at(k)) for k in x_far]

    g_load.wait()
    order = (2, 1, 3, 0)
    p_c = []
    p_y = []

    def pass_on(n):
        k = order[n]
        target = lax.rem(y + k, NY)
        p_c[n].wait_recv()
        pbuf[target, c] = pbuf[target, c] + crecv[n]
        if k:
            p_y.append(send(pbuf.at[target, c], yrecv.at[k - 1], y_at(k)))

    for n in range(NY):
        target = lax.rem(y + order[n], NY)
        both = jnp.dot(
            split_t[...], gv[:, pl.ds(pl.multiple_of(target * 256, 256), 256)],
            preferred_element_type=F32,
        )
        part = both[:RANK] + both[RANK:]
        pbuf[target, 0] = part[:, :128]
        pbuf[target, 1] = part[:, 128:]
        p_c.append(send(pbuf.at[target, mate], crecv.at[n], core))
        if n >= 2:
            pass_on(n - 2)
    pass_on(2)
    pass_on(3)

    for copy in d_z:
        copy.wait_recv()
    total = dzall[0]
    for k in range(1, NZ):
        total = total + dzall[k]
    dgrad[tp, x] = total
    d_ax = [send(dgrad.at[tp, x], dgrad.at[tp, x], x_at(k)) for k in x_far]

    for copy in p_y:
        copy.wait_recv()
    total = pbuf[y, c] + yrecv[0] + yrecv[1] + yrecv[2]
    sbuf[...] = total.reshape(NZ, NX, 8, 128)
    p_x = [send(sbuf.at[:, lax.rem(x + k, NX)], xrecv.at[k - 1], x_at(k)) for k in x_far]

    for copy in d_ax:
        copy.wait_recv()
    d_at = [send(dgrad.at[tp], dgrad.at[tp], tp_at(k)) for k in range(1, 8)]

    for copy in p_x:
        copy.wait_recv()
    tbuf[...] = sbuf[:, x] + xrecv[0] + xrecv[1] + xrecv[2]
    p_z = [send(tbuf.at[lax.rem(z + k, NZ)], zrecv.at[k - 1], z_at(k)) for k in z_far]
    for copy in small_loads:
        copy.wait()
    for copy in p_z:
        copy.wait_recv()
    projected = tbuf[z]
    for k in range(NZ - 1):
        projected = projected + zrecv[k]
    mean_new, second_new, direction = moments(meanv[...], secondv[...], projected)
    dirb[z, x] = direction
    a_z = [send(dirb.at[z, x], dirb.at[z, x], z_at(k)) for k in z_far]
    meanv[...] = mean_new
    secondv[...] = second_new
    outs = [fetch(meanv, mean_out), fetch(secondv, second_out)]

    for copy in d_at:
        copy.wait_recv()
    for t in range(NY * NC):
        for q in range(2):
            cols = slice(256 * t + 128 * q, 256 * t + 128 * (q + 1))
            grad = jnp.concatenate([dgrad[t, q], dgrad[t, 2 + q]], axis=0)
            _, _, step = moments(dmeanv[:, cols], dsecondv[:, cols], grad)
            dstepv[:, cols] = step
            dcopyv[:, cols] = (dmasterv[:, cols] - LEARN_RATE * step).astype(BF16)
    outs += [fetch(dstepv, dstep_out), fetch(dcopyv, dcopy_out)]

    for copy in a_z:
        copy.wait_recv()
    a_x = [send(dirb.at[:, x], dirb.at[:, x], x_at(k)) for k in x_far]
    for copy in m_x:
        copy.wait_recv()
    for copy in a_x:
        copy.wait_recv()

    high, low = split_two(dirb[...].reshape(RANK, 128))
    rhs = jnp.concatenate([high, low], axis=1)
    squares = jnp.zeros((8, 128), F32)
    for i in range(NZ):
        both = jnp.dot(fv[i].reshape(256, RANK), rhs, preferred_element_type=F32)
        part = both[:, :128] + both[:, 128:]
        ubuf[256 * i : 256 * (i + 1), :] = part
        squares = squares + jnp.sum((part * part).reshape(32, 8, 128), axis=0)
    sqb[tp] = squares
    s_t = [send(sqb.at[tp], sqb.at[tp], tp_at(k)) for k in range(1, 8)]
    for copy in s_t:
        copy.wait_recv()
    whole = sqb[0]
    for k in range(1, NY * NC):
        whole = whole + sqb[k]
    mean_square = jnp.sum(whole, axis=(0, 1), keepdims=True) / (D * GW)
    scale = lax.rsqrt(mean_square + RMS_EPS)
    fs = z * NX + x
    step = ubuf[pl.ds(pl.multiple_of(fs * 64, 64), 64), :] * scale
    stepv[...] = step
    newv[...] = mv[z, x] - LEARN_RATE * step
    outs += [fetch(stepv, step_out), fetch(newv, new_out)]
    for i in range(NZ):
        rows = slice(256 * i, 256 * (i + 1))
        step = ubuf[rows, :] * scale
        copyv[rows, :] = (mv[i].reshape(256, 128) - LEARN_RATE * step).astype(BF16)
    outs += [fetch(copyv, copy_out)]
    for copy in sends:
        copy.wait_send()
    for copy in outs:
        copy.wait()


def local(
    saved_input, value_cotangent, decay_cotangent, value_master, value_factor, value_mean,
    value_second, decay_master, decay_mean, decay_second,
):
    shape = jax.ShapeDtypeStruct
    any_spec = pl.BlockSpec(memory_space=pl.ANY)
    scratch = [
        ((TOK, D), BF16), ((TOK, GW), BF16), ((HG, TOK), BF16), ((NZ, NX, 64, RANK), BF16),
        ((NZ, NX, 64, 128), F32), ((8, 128), F32), ((8, 128), F32),
        ((HG, D), F32), ((HG, D), F32), ((HG, D), F32),
        ((TOK, RANK), F32), ((2 * RANK, TOK), BF16), ((NY, NC, RANK, 128), F32),
        ((NY, RANK, 128), F32), ((NY - 1, RANK, 128), F32), ((NZ, NX, 8, 128), F32),
        ((NX - 1, NZ, 8, 128), F32), ((NZ, 8, 128), F32), ((NZ - 1, 8, 128), F32),
        ((NZ, NX, 8, 128), F32), ((D, 128), F32), ((NY * NC, 8, 128), F32),
        ((HG, D), F32), ((NY, NC, NX, 8, 128), F32), ((NY, NX, 8, 128), F32),
        ((NY - 1, NX, 8, 128), F32), ((NX, 8, 128), F32), ((NX - 1, 8, 128), F32),
        ((NZ, 8, 128), F32), ((NY * NC, NX, 8, 128), F32),
        ((64, 128), F32), ((64, 128), F32), ((D, 128), BF16), ((HG, D), F32), ((HG, D), BF16),
    ]
    outs = pl.pallas_call(
        kernel,
        out_shape=(
            shape((64, 128), F32), shape((64, 128), F32), shape((D, 128), BF16),
            shape((8, 128), F32), shape((8, 128), F32), shape((HG, D), F32), shape((HG, D), BF16),
        ),
        in_specs=[any_spec] * 10,
        out_specs=(any_spec,) * 7,
        scratch_shapes=[pltpu.VMEM(*s) for s in scratch]
        + [
            pltpu.SemaphoreType.DMA((20,)),
            pltpu.SemaphoreType.DMA((N_REMOTE,)),
            pltpu.SemaphoreType.DMA((N_REMOTE,)),
        ],
        compiler_params=pltpu.CompilerParams(
            collective_id=0, has_side_effects=True, vmem_limit_bytes=56 * 1024 * 1024
        ),
    )(
        saved_input, value_cotangent, decay_cotangent.T, value_master, value_factor, value_mean,
        value_second, decay_master.T, decay_mean.T, decay_second.T,
    )
    return (*outs[:5], outs[5].T, outs[6].T)


def solution(mesh):
    split = Mesh(mesh.devices.reshape(NZ, NX, NY, NC), FS_TP)
    return jax.shard_map(
        local,
        mesh=split,
        in_specs=(
            P(FS_TP, None), P(FS_TP, None), P(FS_TP, None), P(FS, TP), P(FS, None), P(FS, TP),
            P(FS, TP), P(), P(), P(),
        ),
        out_specs=(P(FS, TP), P(FS, TP), P(None, TP), P(FS, TP), P(FS, TP), P(), P()),
        check_vma=False,
    )
```
